128 devices in a mesh: fs: 16 (over z, y), rep: 4 (over x), tp: 2 (over core).
Axes of the slice: x: 4, y: 4, z: 4, core: 2. Of those that a mesh axis runs over, the one named last changes fastest.
Arguments:
- saved_latent: bfloat16 [49152, 2048], P(('fs', 'rep')), may hold values from -6 to 6
- query_cotangent: bfloat16 [49152, 3072], P(('fs', 'rep'), 'tp'), may hold values from -6 to 6
- mix_cotangent: bfloat16 [49152, 4096], P(('fs', 'rep')), may hold values from -6 to 6
- head_outputs: bfloat16 [49152, 2048], P(('fs', 'rep'), 'tp'), may hold values from -6 to 6
- query_weight: float32 [2048, 3072], P('fs', 'tp'), may hold values from -0.125 to 0.125
- out_weight: float32 [4096, 2048], P('fs', 'tp'), may hold values from -0.125 to 0.125
- query_basis: bfloat16 [2048, 256], replicated, may hold values from -0.125 to 0.125
- out_basis: bfloat16 [4096, 256], replicated, may hold values from -0.09375 to 0.09375
- query_mean: float32 [256, 3072], P('fs', 'tp'), may hold values from -3 to 3
- query_var: float32 [256, 3072], P('fs', 'tp'), may hold values from 0.1 to 1
- out_mean: float32 [256, 2048], P('fs', 'tp'), may hold values from -3 to 3
- out_var: float32 [256, 2048], P('fs', 'tp'), may hold values from 0.1 to 1
Outputs:
- query_step: float32 [2048, 3072], P('fs', 'tp')
- out_step: float32 [4096, 2048], P('fs', 'tp')
- query_copy: bfloat16 [2048, 3072], P('fs', 'tp')
- out_copy: bfloat16 [4096, 2048], P('fs', 'tp')
The draws below stay inside these ranges and needn't reach their ends.
All inputs are finite; a program needn't handle non-finite values.
Results may differ from the reference program's by a relative error of at most 0.001.
Values sent between devices are 32-bit elements; how exact they have to be, the bound alone decides.
No kernel may reach another device: no remote copies, remote signals or barrier semaphores. Data moves between devices by JAX's collectives and lax.ppermute only.
A program may use at most 128 MiB of HBM per device.

```python
import math
import jax
import jax.numpy as jnp
from jax import lax

D = 4096
QLORA = 2048
RANK = 256
TOKENS = 49152
QCOLS = 3072
HV = 2048


def block_scale(key, shape, shards, smallest, largest):
    loudness, own = 1.0, jax.random.fold_in(key, 6)
    for position, shards_of in shards:
        draws = jnp.exp(jax.random.uniform(jax.random.fold_in(own, position), (shards_of,), jnp.float32, smallest / len(shards), largest / len(shards)))
        loudness = loudness * jnp.repeat(draws, shape[position] // shards_of).reshape([-1 if axis == position else 1 for axis in range(len(shape))])
    return loudness


def noise(own_key, dims, deviation, limit, cuts=(), kind=jnp.bfloat16):
    drawn = jax.random.normal(own_key, dims, jnp.float32) * deviation
    if len(cuts) > 0:
        drawn = block_scale(own_key, dims, cuts, -0.22, 0.18) * drawn
    return jnp.clip(drawn, min=-limit, max=limit).astype(kind)


def setup_inputs(seed: int = 0) -> dict:
    streams_of = jax.random.split(jax.random.key(seed), 13)
    saved_latent = noise(streams_of[0], (TOKENS, QLORA), 1.0, 6.0, ((0, 64),))
    query_cotangent = noise(streams_of[1], (TOKENS, QCOLS), 1.0, 6.0, ((0, 64), (1, 2)))
    mix_cotangent = noise(streams_of[2], (TOKENS, D), 1.0, 6.0, ((0, 64),))
    head_outputs = noise(streams_of[3], (TOKENS, HV), 1.0, 6.0, ((0, 64), (1, 2)))
    query_weight = noise(streams_of[4], (QLORA, QCOLS), QLORA ** -0.5, 0.125, ((0, 16), (1, 2)), jnp.float32)
    out_weight = noise(streams_of[5], (D, HV), HV ** -0.5, 0.125, ((0, 16), (1, 2)), jnp.float32)
    query_basis = noise(streams_of[6], (QLORA, RANK), QLORA ** -0.5, 0.125)
    out_basis = noise(streams_of[7], (D, RANK), D ** -0.5, 0.09375)
    query_mean = noise(streams_of[8], (RANK, QCOLS), 0.5, 3.0, ((0, 16), (1, 2)), jnp.float32)
    query_var = jnp.clip(jnp.exp(math.log(1.0) - 2.3025851 * jax.random.uniform(streams_of[9], (RANK, QCOLS), jnp.float32) ** block_scale(streams_of[9], (RANK, QCOLS), ((0, 16), (1, 2)), -0.2, 0.2)), 0.1, 1.0)
    out_mean = noise(streams_of[10], (RANK, HV), 0.5, 3.0, ((0, 16), (1, 2)), jnp.float32)
    out_var = jnp.clip(jnp.exp(math.log(1.0) - 2.3025851 * jax.random.uniform(streams_of[11], (RANK, HV), jnp.float32) ** block_scale(streams_of[11], (RANK, HV), ((0, 16), (1, 2)), -0.2, 0.2)), 0.1, 1.0)
    return dict(saved_latent=saved_latent, query_cotangent=query_cotangent, mix_cotangent=mix_cotangent, head_outputs=head_outputs, query_weight=query_weight, out_weight=out_weight, query_basis=query_basis, out_basis=out_basis, query_mean=query_mean, query_var=query_var, out_mean=out_mean, out_var=out_var)


def token_sum(left, right):
    return lax.dot_general(left, right, (((0,), (0,)), ((), ())), preferred_element_type=jnp.float32)

def project(basis, grad):
    return lax.dot_general(basis.astype(jnp.float32), grad, (((0,), (0,)), ((), ())), precision=lax.Precision.HIGHEST)

def moment_direction(proj, mean, var):
    scale = 1.0 / jnp.maximum(jnp.sqrt(jnp.mean(proj * proj)), 1.0)
    scaled = scale * proj
    new_mean = 0.8 * mean + 0.2 * scaled
    new_var = 0.9 * var + 0.1 * scaled * scaled
    return new_mean / jnp.sqrt(new_var)

def reference(saved_latent, query_cotangent, mix_cotangent, head_outputs, query_weight, out_weight, query_basis, out_basis, query_mean, query_var, out_mean, out_var):
    query_grad = token_sum(saved_latent, query_cotangent)
    out_grad = token_sum(mix_cotangent, head_outputs)
    query_dir = moment_direction(project(query_basis, query_grad), query_mean, query_var)
    out_dir = moment_direction(project(out_basis, out_grad), out_mean, out_var)
    query_step = jnp.dot(query_basis.astype(jnp.float32), query_dir, precision=lax.Precision.HIGHEST)
    out_step = jnp.dot(out_basis.astype(jnp.float32), out_dir, precision=lax.Precision.HIGHEST)
    query_copy = (query_weight - 0.05 * query_step).astype(jnp.bfloat16)
    out_copy = (out_weight - 0.05 * out_step).astype(jnp.bfloat16)
    return (query_step, out_step, query_copy, out_copy)
```

```python
import functools

import jax
import jax.numpy as jnp
from jax import lax
from jax.experimental import pallas as pl
from jax.experimental.pallas import tpu as pltpu
from jax.sharding import PartitionSpec as P

F32 = jnp.float32
BF16 = jnp.bfloat16
STEPS = 3


def halves(value):
    high = value.astype(BF16)
    return high, (value - high.astype(F32)).astype(BF16)


def over_tokens(left, right):
    return lax.dot_general(left, right, (((0,), (0,)), ((), ())), preferred_element_type=F32)


def early_kernel(parts, rows, latent, cot, mix, heads, qbasis, obasis, out):
    step = pl.program_id(0)

    def one(tokens, basis, other, start):
        low_rank = jnp.dot(tokens[...], basis[...], preferred_element_type=F32)
        high, low = halves(low_rank)
        width = other.shape[1] // parts
        for part in range(parts):
            columns = other[:, part * width : (part + 1) * width]
            term = over_tokens(high, columns) + over_tokens(low, columns)
            term = term.reshape(term.shape[0] // rows, rows, width)
            spot = (slice(None), part, slice(None), slice(start, start + width))

            @pl.when(step == 0)
            def _():
                out[spot] = term

            @pl.when(step > 0)
            def _():
                out[spot] += term

    one(latent, qbasis, cot, 0)
    one(mix, obasis, heads, cot.shape[1] // parts)


def early(latent, cot, mix, heads, qbasis, obasis, blocks, parts):
    rows = qbasis.shape[1] // blocks
    wide = (cot.shape[1] + heads.shape[1]) // parts
    tokens = latent.shape[0] // STEPS
    moving = [pl.BlockSpec((tokens, a.shape[1]), lambda i: (i, 0)) for a in (latent, cot, mix, heads)]
    held = [pl.BlockSpec(a.shape, lambda i: (0, 0)) for a in (qbasis, obasis)]
    shape = (blocks, parts, rows, wide)
    return pl.pallas_call(
        functools.partial(early_kernel, parts, rows),
        grid=(STEPS,),
        in_specs=moving + held,
        out_specs=pl.BlockSpec(shape, lambda i: (0, 0, 0, 0)),
        out_shape=jax.ShapeDtypeStruct(shape, F32),
        compiler_params=pltpu.CompilerParams(vmem_limit_bytes=48 << 20),
        cost_estimate=pl.CostEstimate(flops=4_500_000_000, bytes_accessed=19_000_000, transcendentals=0),
        name="early",
    )(latent, cot, mix, heads, qbasis, obasis)


def lanes(value):
    return jnp.sum(value.reshape(value.shape[0], value.shape[1] // 128, 128), axis=(0, 1)).reshape(1, 128)


def total_kernel(split, copies, terms, proj, squares):
    step = pl.program_id(0)
    part = jnp.sum(terms[...], axis=0)

    @pl.when(step == 0)
    def _():
        proj[...] = part

    @pl.when(step > 0)
    def _():
        proj[...] += part

    @pl.when(step == pl.num_programs(0) - 1)
    def _():
        whole = proj[...]
        square = whole * whole
        mine = jnp.concatenate([lanes(square[:, :split]), lanes(square[:, split:])], axis=0)
        squares[...] = jnp.broadcast_to(mine, (copies, 2, 128))


def total(terms, split, copies):
    count, rows, wide = terms.shape
    chunk = count // 4
    return pl.pallas_call(
        functools.partial(total_kernel, split, copies),
        grid=(4,),
        in_specs=[pl.BlockSpec((chunk, rows, wide), lambda i: (i, 0, 0))],
        out_specs=[
            pl.BlockSpec((rows, wide), lambda i: (0, 0)),
            pl.BlockSpec((copies, 2, 128), lambda i: (0, 0, 0)),
        ],
        out_shape=[
            jax.ShapeDtypeStruct((rows, wide), F32),
            jax.ShapeDtypeStruct((copies, 2, 128), F32),
        ],
        name="total",
    )(terms)


def direction_kernel(split, counts, squares, proj, qmean, qvar, omean, ovar, out):
    sums = jnp.sum(jnp.sum(squares[...], axis=0), axis=1, keepdims=True)
    part = lax.axis_index("rep")

    def one(index, start, width, mean, var):
        spot = pl.ds(pl.multiple_of(part * width, 128), width)
        scale = 1.0 / jnp.maximum(jnp.sqrt(sums[index : index + 1] / counts[index]), 1.0)
        scaled = scale * proj[:, start : start + width]
        new_mean = 0.8 * mean[:, spot] + 0.2 * scaled
        new_var = 0.9 * var[:, spot] + 0.1 * scaled * scaled
        return new_mean / jnp.sqrt(new_var)

    wide = proj.shape[1]
    both = jnp.concatenate(
        [one(0, 0, split, qmean, qvar), one(1, split, wide - split, omean, ovar)], axis=1
    )
    out[...] = jnp.broadcast_to(both, out.shape)


def direction(squares, proj, qmean, qvar, omean, ovar, split, counts, copies):
    return pl.pallas_call(
        functools.partial(direction_kernel, split, counts),
        out_shape=jax.ShapeDtypeStruct((copies, *proj.shape), F32),
        name="direction",
    )(squares, proj, qmean, qvar, omean, ovar)


def late_kernel(split, dirs, qbasis, obasis, qweight, oweight, qstep, ostep, qcopy, ocopy):
    def one(basis, start, width, weight, step, copy):
        whole = dirs[:, 0, :, start : start + width]
        high, low = halves(whole.reshape(whole.shape[0] * whole.shape[1], width))
        value = jnp.dot(basis[...], high, preferred_element_type=F32)
        value += jnp.dot(basis[...], low, preferred_element_type=F32)
        step[...] = value
        copy[...] = (weight[...] - 0.05 * value).astype(BF16)

    one(qbasis, 0, split, qweight, qstep, qcopy)
    one(obasis, split, dirs.shape[3] - split, oweight, ostep, ocopy)


def late(dirs, qbasis, obasis, qweight, oweight, split):
    blocks, parts, rows, wide = dirs.shape
    qspec = pl.BlockSpec((qweight.shape[0], split), lambda i: (0, i))
    ospec = pl.BlockSpec((oweight.shape[0], wide - split), lambda i: (0, i))
    return pl.pallas_call(
        functools.partial(late_kernel, split),
        grid=(parts,),
        in_specs=[
            pl.BlockSpec((blocks, 1, rows, wide), lambda i: (0, i, 0, 0)),
            pl.BlockSpec(qbasis.shape, lambda i: (0, 0)),
            pl.BlockSpec(obasis.shape, lambda i: (0, 0)),
            qspec,
            ospec,
        ],
        out_specs=[qspec, ospec, qspec, ospec],
        out_shape=[
            jax.ShapeDtypeStruct(qweight.shape, F32),
            jax.ShapeDtypeStruct(oweight.shape, F32),
            jax.ShapeDtypeStruct(qweight.shape, BF16),
            jax.ShapeDtypeStruct(oweight.shape, BF16),
        ],
        name="late",
    )(dirs, qbasis, obasis, qweight, oweight)


def on_device(
    saved_latent,
    query_cotangent,
    mix_cotangent,
    head_outputs,
    query_weight,
    out_weight,
    query_basis,
    out_basis,
    query_mean,
    query_var,
    out_mean,
    out_var,
):
    blocks, parts, cores = (lax.axis_size(a) for a in ("fs", "rep", "tp"))
    owners = blocks * parts
    position = lax.axis_index("fs")
    query_rows, out_rows = query_weight.shape[0], out_weight.shape[0]
    query_local = lax.dynamic_slice_in_dim(query_basis, position * query_rows, query_rows, 0)
    out_local = lax.dynamic_slice_in_dim(out_basis, position * out_rows, out_rows, 0)
    split = query_cotangent.shape[1] // parts
    rank = query_basis.shape[1]
    counts = (
        float(rank * query_cotangent.shape[1] * cores),
        float(rank * head_outputs.shape[1] * cores),
    )
    terms = early(
        saved_latent, query_cotangent, mix_cotangent, head_outputs, query_basis, out_basis, blocks, parts
    )
    rows, wide = terms.shape[2:]
    sent = lax.all_to_all(terms.reshape(owners, rows, wide), ("fs", "rep"), 0, 0, tiled=True)
    proj, squares = total(sent, split, owners * cores)
    squares = lax.all_to_all(squares, ("fs", "rep", "tp"), 0, 0, tiled=True)
    mine = direction(
        squares, proj, query_mean, query_var, out_mean, out_var, split, counts, owners
    )
    dirs = lax.all_to_all(mine, ("fs", "rep"), 0, 0, tiled=True)
    dirs = dirs.reshape(blocks, parts, rows, wide)
    return tuple(late(dirs, query_local, out_local, query_weight, out_weight, split))


def solution(mesh):
    placed = (
        P(("fs", "rep"), None),
        P(("fs", "rep"), "tp"),
        P(("fs", "rep"), None),
        P(("fs", "rep"), "tp"),
        P("fs", "tp"),
        P("fs", "tp"),
        P(),
        P(),
        P("fs", "tp"),
        P("fs", "tp"),
        P("fs", "tp"),
        P("fs", "tp"),
    )
    return jax.shard_map(
        on_device,
        mesh=mesh,
        in_specs=placed,
        out_specs=(P("fs", "tp"), P("fs", "tp"), P("fs", "tp"), P("fs", "tp")),
        check_vma=False,
    )
```

```python
import functools

import jax
import jax.numpy as jnp
from jax import lax
from jax.experimental import pallas as pl
from jax.experimental.pallas import tpu as pltpu
from jax.sharding import PartitionSpec as P


F32 = jnp.float32
BF16 = jnp.bfloat16
AXES = ("fs", "rep", "tp")
RING = 4
STEPS = 4


def first(place, core):
    gray, top = (place // 2) ^ (place % 2), place // 2
    return gray + core * (top - gray)


def second(place, core):
    return first(place, 1 - core)


def place_of(one, two, core):
    return 2 * (two + core * (one - two)) + (one ^ two)


def devices():
    return [(z, y, x, c) for z in range(RING) for y in range(RING) for x in range(RING) for c in range(2)]


def number(z, y, x, core):
    return ((z * RING + y) * RING + x) * 2 + core


def partners(phase, offset):
    pairs = []
    for *spots, core in devices():
        bits = (offset & 1, (offset >> 1) & 1, offset >> 2)
        there = []
        for spot, bit in zip(spots, bits):
            one, two = first(spot, core), second(spot, core)
            there.append(place_of(one ^ bit, two, core) if phase == 1 else place_of(one, two ^ bit, core))
        pairs.append((number(*spots, core), number(*there, core)))
    return pairs


def first_groups():
    groups = {}
    for z, y, x, core in devices():
        key = tuple(second(s, core) for s in (x, y, z)) + (core,)
        slot = sum(first(s, core) << k for s, k in ((x, 2), (y, 1), (z, 0)))
        groups.setdefault(key, {})[slot] = number(z, y, x, core)
    return [[g[s] for s in range(8)] for g in groups.values()]


def here():
    block = lax.axis_index("fs")
    return block // RING, block % RING, lax.axis_index("rep"), lax.axis_index("tp")


def halves(value):
    high = value.astype(BF16)
    return high, (value - high.astype(F32)).astype(BF16)


def params(mebibytes):
    return pltpu.CompilerParams(vmem_limit_bytes=mebibytes << 20)


def cost(micros):
    return pl.CostEstimate(flops=int(micros * 1e8), bytes_accessed=int(micros * 1e6), transcendentals=0)


def low_rank_kernel(latent, mix, qbasis, obasis, qout, oout, qacc, oacc):
    step, last = pl.program_id(0), pl.num_programs(0) - 1
    for tokens, basis, acc, out in ((latent, qbasis, qacc, qout), (mix, obasis, oacc, oout)):
        term = jnp.dot(tokens[...], basis[...], preferred_element_type=F32)

        @pl.when(step == 0)
        def _():
            acc[...] = term

        @pl.when(step > 0)
        def _():
            acc[...] += term

        @pl.when(step == last)
        def _():
            high, low = halves(acc[...].T)
            out[0] = high
            out[1] = low


def low_rank(latent, mix, qbasis, obasis):
    tokens, rank = latent.shape[0], qbasis.shape[1]
    wide = [pl.BlockSpec((tokens, a.shape[1] // STEPS), lambda i: (0, i)) for a in (latent, mix)]
    tall = [pl.BlockSpec((a.shape[0] // STEPS, rank), lambda i: (i, 0)) for a in (qbasis, obasis)]
    shape = jax.ShapeDtypeStruct((2, rank, tokens), BF16)
    return pl.pallas_call(
        low_rank_kernel,
        grid=(STEPS,),
        in_specs=wide + tall,
        out_specs=[pl.BlockSpec(shape.shape, lambda i: (0, 0, 0))] * 2,
        out_shape=[shape, shape],
        scratch_shapes=[pltpu.VMEM((tokens, rank), F32)] * 2,
        compiler_params=params(24),
        cost_estimate=cost(5),
        name="low_rank",
    )(latent, mix, qbasis, obasis)


def part_of(flip):
    def index(i):
        _, _, x, core = here()
        return place_of(first(x, core) ^ flip, i, core)

    return index


def rows_of(spot, pair):
    z, y, _, core = here()
    there_y = place_of(first(y, core) ^ (spot >> 1), pair >> 1, core)
    there_z = place_of(first(z, core) ^ (spot & 1), pair & 1, core)
    return there_z * RING + there_y


def blocks_kernel(rows, qlow, olow, cot, heads, *rest):
    outs, (qterm, oterm) = rest[:4], rest[4:]
    for low, other, term in ((qlow, cot, qterm), (olow, heads, oterm)):
        value = jnp.dot(low[0], other[...], preferred_element_type=F32)
        term[...] = value + jnp.dot(low[1], other[...], preferred_element_type=F32)
    width = cot.shape[1]
    for spot in range(4):
        for pair in range(4):
            at = pl.ds(pl.multiple_of(rows_of(spot, pair) * rows, rows), rows)
            outs[spot][pair, :, :width] = qterm[at, :]
            outs[spot][pair, :, width:] = oterm[at, :]


def blocks(qlow, olow, cot, heads, flip):
    rank, tokens = qlow.shape[1:]
    rows = rank // (RING * RING)
    qwide, owide = cot.shape[1] // RING, heads.shape[1] // RING
    index = part_of(flip)
    shape = (8, rows, qwide + owide)
    return pl.pallas_call(
        functools.partial(blocks_kernel, rows),
        grid=(2,),
        in_specs=[
            pl.BlockSpec(qlow.shape, lambda i: (0, 0, 0)),
            pl.BlockSpec(olow.shape, lambda i: (0, 0, 0)),
            pl.BlockSpec((tokens, qwide), lambda i: (0, index(i))),
            pl.BlockSpec((tokens, owide), lambda i: (0, index(i))),
        ],
        out_specs=[pl.BlockSpec((4, *shape[1:]), lambda i: (i, 0, 0))] * 4,
        out_shape=[jax.ShapeDtypeStruct(shape, F32)] * 4,
        scratch_shapes=[pltpu.VMEM((rank, qwide), F32), pltpu.VMEM((rank, owide), F32)],
        compiler_params=params(16),
        cost_estimate=cost(2),
        name=f"blocks{flip}",
    )(qlow, olow, cot, heads)


def tree(values):
    while len(values) > 1:
        values = [a + b for a, b in zip(values[::2], values[1::2])]
    return values[0]


def lanes(value):
    rows, wide = value.shape
    total = jnp.sum(value, axis=0, keepdims=True)
    return sum(total[:, k : k + 128] for k in range(0, wide, 128))


def total_kernel(*refs):
    refs[8][...] = tree([r[...] for r in refs[:8]])


def squares_kernel(split, *refs):
    proj, squares = refs[8:10]
    value = tree([r[...] for r in refs[:8]])
    proj[...] = value
    value = value.reshape(value.shape[0] * value.shape[1], value.shape[2])
    square = value * value
    mine = jnp.concatenate([lanes(square[:, :split]), lanes(square[:, split:])], axis=0)
    squares[...] = jnp.broadcast_to(mine, squares.shape)


def total(terms):
    return pl.pallas_call(
        total_kernel,
        grid=(2,),
        in_specs=[pl.BlockSpec((4, *terms[0].shape[1:]), lambda i: (i, 0, 0))] * 8,
        out_specs=pl.BlockSpec((4, *terms[0].shape[1:]), lambda i: (i, 0, 0)),
        out_shape=jax.ShapeDtypeStruct(terms[0].shape, F32),
        compiler_params=params(8),
        cost_estimate=cost(1.5),
        name="total",
    )(*terms)


def total_squares(terms, split):
    return pl.pallas_call(
        functools.partial(squares_kernel, split),
        out_shape=[
            jax.ShapeDtypeStruct(terms[0].shape, F32),
            jax.ShapeDtypeStruct((8, 2, 128), F32),
        ],
        compiler_params=params(10),
        cost_estimate=cost(1.5),
        name="total_squares",
    )(*terms)


def moments_kernel(qmean, qvar, omean, ovar, out):
    _, _, x, core = here()
    for part in range(2):
        index = place_of(first(x, core), part, core)
        start = 0
        for source in ((qmean, qvar), (omean, ovar)):
            width = source[0].shape[1] // RING
            at = pl.ds(pl.multiple_of(index * width, 128), width)
            for which in range(2):
                out[which, part, :, start : start + width] = source[which][:, at]
            start += width


def moments(qmean, qvar, omean, ovar):
    wide = (qmean.shape[1] + omean.shape[1]) // RING
    return pl.pallas_call(
        moments_kernel,
        out_shape=jax.ShapeDtypeStruct((2, 2, qmean.shape[0], wide), F32),
        compiler_params=params(4),
        cost_estimate=cost(1),
        name="moments",
    )(qmean, qvar, omean, ovar)


def direction_kernel(split, counts, mine, other, proj, *refs):
    moved, out = refs[:4], refs[4]
    z, y, _, core = here()
    own = second(y, core) * 2 + second(z, core)
    sums = jnp.sum(mine[...], axis=0) + jnp.sum(other[...], axis=0)
    sums = jnp.sum(sums, axis=1, keepdims=True)
    scales = [1.0 / jnp.maximum(jnp.sqrt(sums[k : k + 1] / counts[k]), 1.0) for k in range(2)]
    for offset in range(4):
        for part in range(2):
            shard = part * 4 + (own ^ offset)
            for k, at in enumerate((slice(0, split), slice(split, None))):
                scaled = scales[k] * proj[shard, :, at]
                new_mean = 0.8 * moved[offset][0, part, :, at] + 0.2 * scaled
                new_var = 0.9 * moved[offset][1, part, :, at] + 0.1 * scaled * scaled
                out[shard, :, at] = new_mean / jnp.sqrt(new_var)


def direction(mine, other, proj, moved, split, counts):
    return pl.pallas_call(
        functools.partial(direction_kernel, split, counts),
        out_shape=jax.ShapeDtypeStruct(proj.shape, F32),
        compiler_params=params(6),
        cost_estimate=cost(1.5),
        name="direction",
    )(mine, other, proj, *moved)


def late_kernel(rows, split, aliased, *refs):
    dirs, (qbasis, obasis, qweight, oweight) = refs[:4], refs[4:8]
    outs, scratch = refs[8 + aliased : 12 + aliased], refs[12 + aliased :]
    qstep, ostep, qcopy, ocopy = outs
    for spot in range(4):
        for pair in range(4):
            at = pl.ds(pl.multiple_of(rows_of(spot, pair) * rows, rows), rows)
            for ref, value in zip(scratch, halves(dirs[spot][pair])):
                ref[at, :] = value
    wide = scratch[0].shape[1]
    for basis, at, weight, step, copy in (
        (qbasis, slice(0, split), qweight, qstep, qcopy),
        (obasis, slice(split, wide), oweight, ostep, ocopy),
    ):
        value = jnp.dot(basis[...], scratch[0][:, at], preferred_element_type=F32)
        value += jnp.dot(basis[...], scratch[1][:, at], preferred_element_type=F32)
        step[...] = value
        copy[...] = (weight[...] - 0.05 * value).astype(BF16)


def late(dirs, qbasis, obasis, qweight, oweight, split, flip, before=()):
    _, rows, wide = dirs[0].shape
    rank = qbasis.shape[1]
    index = part_of(flip)
    qspec = pl.BlockSpec((qweight.shape[0], split), lambda i: (0, index(i)))
    ospec = pl.BlockSpec((oweight.shape[0], wide - split), lambda i: (0, index(i)))
    return pl.pallas_call(
        functools.partial(late_kernel, rows, split, len(before)),
        grid=(2,),
        in_specs=[pl.BlockSpec((4, rows, wide), lambda i: (i, 0, 0))] * 4
        + [
            pl.BlockSpec((qweight.shape[0], rank), lambda i: (lax.axis_index("fs"), 0)),
            pl.BlockSpec((oweight.shape[0], rank), lambda i: (lax.axis_index("fs"), 0)),
            qspec,
            ospec,
        ]
        + [pl.BlockSpec(memory_space=pl.ANY)] * len(before),
        out_specs=[qspec, ospec, qspec, ospec],
        out_shape=[
            jax.ShapeDtypeStruct(qweight.shape, F32),
            jax.ShapeDtypeStruct(oweight.shape, F32),
            jax.ShapeDtypeStruct(qweight.shape, BF16),
            jax.ShapeDtypeStruct(oweight.shape, BF16),
        ],
        scratch_shapes=[pltpu.VMEM((rank, wide), BF16)] * 2,
        input_output_aliases={8 + k: k for k in range(len(before))},
        compiler_params=params(12),
        cost_estimate=cost(2),
        name=f"late{flip}",
    )(*dirs, qbasis, obasis, qweight, oweight, *before)


def swap(value, phase, offset):
    return lax.ppermute(value, AXES, partners(phase, offset))


def on_device(
    saved_latent,
    query_cotangent,
    mix_cotangent,
    head_outputs,
    query_weight,
    out_weight,
    query_basis,
    out_basis,
    query_mean,
    query_var,
    out_mean,
    out_var,
):
    rank, cores = query_basis.shape[1], lax.axis_size("tp")
    split = query_cotangent.shape[1] // RING
    counts = (
        float(rank * query_cotangent.shape[1] * cores),
        float(rank * head_outputs.shape[1] * cores),
    )
    qlow, olow = low_rank(saved_latent, mix_cotangent, query_basis, out_basis)
    far = blocks(qlow, olow, query_cotangent, head_outputs, 1)
    near = blocks(qlow, olow, query_cotangent, head_outputs, 0)
    held = moments(query_mean, query_var, out_mean, out_var)
    came = {4 + k: swap(far[k], 1, 4 + k) for k in (3, 2, 1, 0)}
    came |= {k: swap(near[k], 1, k) for k in (3, 2, 1)}
    moved = [held] + [swap(held, 2, k) for k in (1, 2, 3)]
    partial = total([near[0]] + [came[k] for k in range(1, 8)])
    proj, squares = total_squares([partial] + [swap(partial, 2, k) for k in range(1, 8)], split)
    mine = lax.all_to_all(squares, AXES, 0, 0, tiled=True, axis_index_groups=first_groups())
    other = lax.ppermute(mine, "tp", [(0, 1), (1, 0)])
    dirs = direction(mine, other, proj, moved, split, counts)
    spread = [dirs] + [swap(dirs, 1, k) for k in range(1, 8)]
    steps = late(spread[:4], query_basis, out_basis, query_weight, out_weight, split, 0)
    return tuple(late(spread[4:], query_basis, out_basis, query_weight, out_weight, split, 1, steps))


def solution(mesh):
    placed = (
        P(("fs", "rep"), None),
        P(("fs", "rep"), "tp"),
        P(("fs", "rep"), None),
        P(("fs", "rep"), "tp"),
        P("fs", "tp"),
        P("fs", "tp"),
        P(),
        P(),
        P("fs", "tp"),
        P("fs", "tp"),
        P("fs", "tp"),
        P("fs", "tp"),
    )
    return jax.shard_map(
        on_device,
        mesh=mesh,
        in_specs=placed,
        out_specs=(P("fs", "tp"), P("fs", "tp"), P("fs", "tp"), P("fs", "tp")),
        check_vma=False,
    )
```

```python
import functools

import jax
import jax.numpy as jnp
from jax import lax
from jax.experimental import pallas as pl
from jax.experimental.pallas import tpu as pltpu
from jax.sharding import PartitionSpec as P


F32 = jnp.float32
BF16 = jnp.bfloat16
AXES = ("fs", "rep", "tp")
RING = 4
FAR = 16
FRONT = 51
STEPS = 4
AHEAD = 24
ORDERS = ((4, 2, 1), (2, 1, 4))


def first(place, core):
    gray, top = (place // 2) ^ (place % 2), place // 2
    return gray + core * (top - gray)


def second(place, core):
    return first(place, 1 - core)


def place_of(one, two, core):
    return 2 * (two + core * (one - two)) + (one ^ two)


def devices():
    return [(z, y, x, c) for z in range(RING) for y in range(RING) for x in range(RING) for c in range(2)]


def number(z, y, x, core):
    return ((z * RING + y) * RING + x) * 2 + core


def partners(phase, offset):
    pairs = []
    for *spots, core in devices():
        bits = (offset & 1, (offset >> 1) & 1, offset >> 2)
        there = []
        for spot, bit in zip(spots, bits):
            one, two = first(spot, core), second(spot, core)
            there.append(place_of(one ^ bit, two, core) if phase == 1 else place_of(one, two ^ bit, core))
        pairs.append((number(*spots, core), number(*there, core)))
    return pairs


def first_groups():
    groups = {}
    for z, y, x, core in devices():
        key = tuple(second(s, core) for s in (x, y, z)) + (core,)
        slot = sum(first(s, core) << k for s, k in ((x, 2), (y, 1), (z, 0)))
        groups.setdefault(key, {})[slot] = number(z, y, x, core)
    return [[g[s] for s in range(8)] for g in groups.values()]


def here():
    block = lax.axis_index("fs")
    return block // RING, block % RING, lax.axis_index("rep"), lax.axis_index("tp")


def halves(value):
    high = value.astype(BF16)
    return high, (value - high.astype(F32)).astype(BF16)


def params(mebibytes):
    return pltpu.CompilerParams(vmem_limit_bytes=mebibytes << 20)


def cost(micros):
    return pl.CostEstimate(flops=int(micros * 1e8), bytes_accessed=int(micros * 1e6), transcendentals=0)


def part_of(flip):
    def index(i):
        _, _, x, core = here()
        return place_of(first(x, core) ^ flip, i, core)

    return index


def rows_of(spot, pair):
    z, y, _, core = here()
    there_y = place_of(first(y, core) ^ (spot >> 1), pair >> 1, core)
    there_z = place_of(first(z, core) ^ (spot & 1), pair & 1, core)
    return there_z * RING + there_y


def spread_rows(rows, qterm, oterm, outs, base):
    width = qterm.shape[1]
    for spot in range(4):
        for pair in range(4):
            at = pl.ds(pl.multiple_of(rows_of(spot, pair) * rows, rows), rows)
            outs[spot][base + pair, :, :width] = qterm[at, :]
            outs[spot][base + pair, :, width:] = oterm[at, :]


def over_tokens(low, other):
    value = jnp.dot(low[0], other, preferred_element_type=F32)
    return value + jnp.dot(low[1], other, preferred_element_type=F32)


def blocks_kernel(rows, flip, qlow, olow, cot, heads, outs, qterm, oterm):
    for part in range(2):
        index = part_of(flip)(part)
        for low, other, term in ((qlow, cot, qterm), (olow, heads, oterm)):
            width = term.shape[1]
            at = pl.ds(pl.multiple_of(index * width, 128), width)
            term[...] = over_tokens(low, other[:, at])
        spread_rows(rows, qterm, oterm, outs, 4 * part)


def front_kernel(rows, latent, mix, qbasis, obasis, cot, heads, *refs):
    qlow, olow, outs = refs[0], refs[1], refs[2:6]
    xs, ms, qs, os, qfar, ofar, total, qterm, oterm, sems = refs[6:]
    copies, waits = [], {}

    def bring(key, source, target):
        waits.setdefault(key, []).append(len(copies))
        copies.append(pltpu.make_async_copy(source, target, sems.at[len(copies)]))

    for name, tokens, basis, inside, beside in (("m", mix, obasis, ms, os), ("x", latent, qbasis, xs, qs)):
        wide = tokens.shape[1] // STEPS
        for k in range(STEPS):
            at = pl.ds(k * wide, wide)
            bring((name, k), basis.at[at, :], beside.at[at, :])
            bring((name, k), tokens.at[:, at], inside.at[:, at])
    for source, target in ((cot, qfar), (heads, ofar)):
        width = target.shape[2]
        for part in range(2):
            at = pl.ds(pl.multiple_of(part_of(1)(part) * width, 128), width)
            bring(part, source.at[:, at], target.at[part])
    begun = 0

    def ahead(upto):
        nonlocal begun
        while begun < min(upto, len(copies)):
            copies[begun].start()
            begun += 1

    def ready(key):
        for k in waits[key]:
            copies[k].wait()
        ahead(max(waits[key]) + 1 + AHEAD)

    apart = lax.axis_index("fs") >= 0
    ahead(AHEAD)
    for name, inside, beside, low in (("m", ms, os, olow), ("x", xs, qs, qlow)):
        wide = inside.shape[1] // STEPS
        for k in range(STEPS):

            @pl.when(apart)
            def _():
                ready((name, k))
                term = jnp.dot(
                    inside[:, k * wide : (k + 1) * wide],
                    beside[k * wide : (k + 1) * wide, :],
                    preferred_element_type=F32,
                )
                if k > 0:
                    term += total[...]
                if k < STEPS - 1:
                    total[...] = term
                else:
                    high, rest = halves(term)
                    low[0] = high.T
                    low[1] = rest.T

    for part in range(2):

        @pl.when(apart)
        def _():
            ready(part)
            qterm[...] = over_tokens(qlow, qfar[part])
            oterm[...] = over_tokens(olow, ofar[part])
            spread_rows(rows, qterm, oterm, outs, 4 * part)


def front(latent, mix, qbasis, obasis, cot, heads):
    tokens, rank = latent.shape[0], qbasis.shape[1]
    rows = rank // (RING * RING)
    qwide, owide = cot.shape[1] // RING, heads.shape[1] // RING
    low = jax.ShapeDtypeStruct((2, rank, tokens), BF16)
    kept = [jax.ShapeDtypeStruct((2, tokens, w), BF16) for w in (qwide, owide)]
    block = jax.ShapeDtypeStruct((8, rows, qwide + owide), F32)
    return pl.pallas_call(
        functools.partial(front_kernel, rows),
        in_specs=[pl.BlockSpec(memory_space=pltpu.HBM)] * 6,
        out_shape=[low, low] + [block] * 4,
        scratch_shapes=[pltpu.VMEM(a.shape, BF16) for a in (latent, mix, qbasis, obasis, *kept)]
        + [pltpu.VMEM((tokens, rank), F32)]
        + [pltpu.VMEM((rank, w), F32) for w in (qwide, owide)]
        + [pltpu.SemaphoreType.DMA((4 * STEPS + 4,))],
        compiler_params=params(FRONT),
        cost_estimate=cost(7),
        name="front",
    )(latent, mix, qbasis, obasis, cot, heads)


def near_kernel(rows, qlow, olow, cot, heads, *refs):
    blocks_kernel(rows, 0, qlow, olow, cot, heads, refs[:4], *refs[4:])


def near_blocks(qlow, olow, cot, heads):
    rank = qlow.shape[1]
    rows = rank // (RING * RING)
    qwide, owide = cot.shape[1] // RING, heads.shape[1] // RING
    block = jax.ShapeDtypeStruct((8, rows, qwide + owide), F32)
    return pl.pallas_call(
        functools.partial(near_kernel, rows),
        out_shape=[block] * 4,
        scratch_shapes=[pltpu.VMEM((rank, w), F32) for w in (qwide, owide)],
        compiler_params=params(FAR),
        cost_estimate=cost(2),
        name="near",
    )(qlow, olow, cot, heads)


def tree(values):
    while len(values) > 1:
        values = [a + b for a, b in zip(values[::2], values[1::2])]
    return values[0]


def lanes(value):
    _, wide = value.shape
    total = jnp.sum(value, axis=0, keepdims=True)
    return sum(total[:, k : k + 128] for k in range(0, wide, 128))


def total_kernel(*refs):
    value = tree([r[...] for r in refs[:8]])
    for half in range(2):
        refs[8 + half][...] = value[4 * half : 4 * half + 4]


def squares_kernel(split, *refs):
    proj, squares = refs[4:]
    for half in range(2):
        proj[4 * half : 4 * half + 4] = refs[2 * half][...] + refs[2 * half + 1][...]
    value = proj[...]
    value = value.reshape(value.shape[0] * value.shape[1], value.shape[2])
    square = value * value
    mine = jnp.concatenate([lanes(square[:, :split]), lanes(square[:, split:])], axis=0)
    squares[...] = jnp.broadcast_to(mine, squares.shape)


def total(terms):
    shape = terms[0].shape
    return pl.pallas_call(
        total_kernel,
        out_shape=[jax.ShapeDtypeStruct((4, *shape[1:]), F32)] * 2,
        compiler_params=params(10),
        cost_estimate=cost(0.5),
        name="total",
    )(*terms)


def total_squares(terms, split):
    return pl.pallas_call(
        functools.partial(squares_kernel, split),
        out_shape=[
            jax.ShapeDtypeStruct((8, *terms[0].shape[1:]), F32),
            jax.ShapeDtypeStruct((8, 2, 128), F32),
        ],
        compiler_params=params(10),
        cost_estimate=cost(0.5),
        name="total_squares",
    )(*terms)


def moments_kernel(qmean, qvar, omean, ovar, out):
    _, _, x, core = here()
    for part in range(2):
        index = place_of(first(x, core), part, core)
        start = 0
        for source in ((qmean, qvar), (omean, ovar)):
            width = source[0].shape[1] // RING
            at = pl.ds(pl.multiple_of(index * width, 128), width)
            for which in range(2):
                out[which, part, :, start : start + width] = source[which][:, at]
            start += width


def moments(qmean, qvar, omean, ovar):
    wide = (qmean.shape[1] + omean.shape[1]) // RING
    return pl.pallas_call(
        moments_kernel,
        out_shape=jax.ShapeDtypeStruct((2, 2, qmean.shape[0], wide), F32),
        compiler_params=params(4),
        cost_estimate=cost(1),
        name="moments",
    )(qmean, qvar, omean, ovar)


def direction_kernel(split, counts, mine, other, proj, *refs):
    moved, out = refs[:4], refs[4]
    z, y, _, core = here()
    own = second(y, core) * 2 + second(z, core)
    sums = jnp.sum(mine[...], axis=0) + jnp.sum(other[...], axis=0)
    sums = jnp.sum(sums, axis=1, keepdims=True)
    scales = [1.0 / jnp.maximum(jnp.sqrt(sums[k : k + 1] / counts[k]), 1.0) for k in range(2)]
    for offset in range(4):
        for part in range(2):
            shard = part * 4 + (own ^ offset)
            for k, at in enumerate((slice(0, split), slice(split, None))):
                scaled = scales[k] * proj[shard, :, at]
                new_mean = 0.8 * moved[offset][0, part, :, at] + 0.2 * scaled
                new_var = 0.9 * moved[offset][1, part, :, at] + 0.1 * scaled * scaled
                out[shard, :, at] = new_mean / jnp.sqrt(new_var)


def direction(mine, other, proj, moved, split, counts):
    return pl.pallas_call(
        functools.partial(direction_kernel, split, counts),
        out_shape=jax.ShapeDtypeStruct(proj.shape, F32),
        compiler_params=params(6),
        cost_estimate=cost(1.5),
        name="direction",
    )(mine, other, proj, *moved)


def late_kernel(rows, split, aliased, *refs):
    dirs, (qbasis, obasis, qweight, oweight) = refs[:4], refs[4:8]
    outs, scratch = refs[8 + aliased : 12 + aliased], refs[12 + aliased :]
    qstep, ostep, qcopy, ocopy = outs
    for spot in range(4):
        for pair in range(4):
            at = pl.ds(pl.multiple_of(rows_of(spot, pair) * rows, rows), rows)
            for ref, value in zip(scratch, halves(dirs[spot][pair])):
                ref[at, :] = value
    wide = scratch[0].shape[1]
    for basis, at, weight, step, copy in (
        (qbasis, slice(0, split), qweight, qstep, qcopy),
        (obasis, slice(split, wide), oweight, ostep, ocopy),
    ):
        value = jnp.dot(basis[...], scratch[0][:, at], preferred_element_type=F32)
        value += jnp.dot(basis[...], scratch[1][:, at], preferred_element_type=F32)
        step[...] = value
        copy[...] = (weight[...] - 0.05 * value).astype(BF16)


def late(dirs, qbasis, obasis, qweight, oweight, split, flip, before=()):
    _, rows, wide = dirs[0].shape
    rank = qbasis.shape[1]
    index = part_of(flip)
    qspec = pl.BlockSpec((qweight.shape[0], split), lambda i: (0, index(i)))
    ospec = pl.BlockSpec((oweight.shape[0], wide - split), lambda i: (0, index(i)))
    return pl.pallas_call(
        functools.partial(late_kernel, rows, split, len(before)),
        grid=(2,),
        in_specs=[pl.BlockSpec((4, rows, wide), lambda i: (i, 0, 0))] * 4
        + [
            pl.BlockSpec((qweight.shape[0], rank), lambda i: (lax.axis_index("fs"), 0)),
            pl.BlockSpec((oweight.shape[0], rank), lambda i: (lax.axis_index("fs"), 0)),
            qspec,
            ospec,
        ]
        + [pl.BlockSpec(memory_space=pl.ANY)] * len(before),
        out_specs=[qspec, ospec, qspec, ospec],
        out_shape=[
            jax.ShapeDtypeStruct(qweight.shape, F32),
            jax.ShapeDtypeStruct(oweight.shape, F32),
            jax.ShapeDtypeStruct(qweight.shape, BF16),
            jax.ShapeDtypeStruct(oweight.shape, BF16),
        ],
        scratch_shapes=[pltpu.VMEM((rank, wide), BF16)] * 2,
        input_output_aliases={8 + k: k for k in range(len(before))},
        compiler_params=params(12),
        cost_estimate=cost(2),
    )(*dirs, qbasis, obasis, qweight, oweight, *before)


def swap(value, phase, offset):
    return lax.ppermute(value, AXES, partners(phase, offset))


def on_device(
    saved_latent,
    query_cotangent,
    mix_cotangent,
    head_outputs,
    query_weight,
    out_weight,
    query_basis,
    out_basis,
    query_mean,
    query_var,
    out_mean,
    out_var,
):
    rank, cores = query_basis.shape[1], lax.axis_size("tp")
    split = query_cotangent.shape[1] // RING
    counts = (
        float(rank * query_cotangent.shape[1] * cores),
        float(rank * head_outputs.shape[1] * cores),
    )
    qlow, olow, *far = front(
        saved_latent, mix_cotangent, query_basis, out_basis, query_cotangent, head_outputs
    )
    near = near_blocks(qlow, olow, query_cotangent, head_outputs)
    held = moments(query_mean, query_var, out_mean, out_var)
    came = {}
    for k in (3, 2, 1, 0):
        came[4 + k] = swap(far[k], 1, 4 + k)
    came |= {k: swap(near[k], 1, k) for k in (3, 2, 1)}
    moved = [swap(held, 2, k) for k in (1, 2, 3)]
    near, came, moved = lax.optimization_barrier((near, came, moved))
    moved = [held] + moved
    chains = list(total([near[0]] + [came[k] for k in range(1, 8)]))
    for step in range(3):
        others = [swap(v, 2, order[step]) for v, order in zip(chains, ORDERS)]
        if step < 2:
            chains = [v + w for v, w in zip(chains, others)]
    last = [v for pair in zip(chains, others) for v in pair]
    proj, squares = total_squares(last, split)
    mine = lax.all_to_all(squares, AXES, 0, 0, tiled=True, axis_index_groups=first_groups())
    other = lax.ppermute(mine, "tp", [(0, 1), (1, 0)])
    dirs = direction(mine, other, proj, moved, split, counts)
    spread = [dirs] + [swap(dirs, 1, k) for k in range(1, 8)]
    steps = late(spread[:4], query_basis, out_basis, query_weight, out_weight, split, 0)
    return tuple(late(spread[4:], query_basis, out_basis, query_weight, out_weight, split, 1, steps))


def solution(mesh):
    placed = (
        P(("fs", "rep"), None),
        P(("fs", "rep"), "tp"),
        P(("fs", "rep"), None),
        P(("fs", "rep"), "tp"),
        P("fs", "tp"),
        P("fs", "tp"),
        P(),
        P(),
        P("fs", "tp"),
        P("fs", "tp"),
        P("fs", "tp"),
        P("fs", "tp"),
    )
    return jax.shard_map(
        on_device,
        mesh=mesh,
        in_specs=placed,
        out_specs=(P("fs", "tp"), P("fs", "tp"), P("fs", "tp"), P("fs", "tp")),
        check_vma=False,
    )
```

```python
import functools

import jax
import jax.numpy as jnp
from jax import lax
from jax.experimental import pallas as pl
from jax.experimental.pallas import tpu as pltpu
from jax.sharding import PartitionSpec as P


F32 = jnp.float32
BF16 = jnp.bfloat16
AXES = ("fs", "rep", "tp")
RING = 4
FAR = 16
FRONT = 51
STEPS = 4
AHEAD = 24
GATHER = (7, 6, 1, 5, 2, 3, 4)
SPREAD = (3, 1, 6, 2, 5, 7, 4)
ORDERS = ((4, 2, 1), (2, 1, 4))


def first(place, core):
    gray, top = (place // 2) ^ (place % 2), place // 2
    return gray + core * (top - gray)


def second(place, core):
    return first(place, 1 - core)


def place_of(one, two, core):
    return 2 * (two + core * (one - two)) + (one ^ two)


def devices():
    return [(z, y, x, c) for z in range(RING) for y in range(RING) for x in range(RING) for c in range(2)]


def number(z, y, x, core):
    return ((z * RING + y) * RING + x) * 2 + core


def partners(phase, offset):
    pairs = []
    for *spots, core in devices():
        bits = (offset & 1, (offset >> 1) & 1, offset >> 2)
        there = []
        for spot, bit in zip(spots, bits):
            one, two = first(spot, core), second(spot, core)
            there.append(place_of(one ^ bit, two, core) if phase == 1 else place_of(one, two ^ bit, core))
        pairs.append((number(*spots, core), number(*there, core)))
    return pairs


def first_groups():
    groups = {}
    for z, y, x, core in devices():
        key = tuple(second(s, core) for s in (x, y, z)) + (core,)
        slot = sum(first(s, core) << k for s, k in ((x, 2), (y, 1), (z, 0)))
        groups.setdefault(key, {})[slot] = number(z, y, x, core)
    return [[g[s] for s in range(8)] for g in groups.values()]


def here():
    block = lax.axis_index("fs")
    return block // RING, block % RING, lax.axis_index("rep"), lax.axis_index("tp")


def halves(value):
    high = value.astype(BF16)
    return high, (value - high.astype(F32)).astype(BF16)


def params(mebibytes):
    return pltpu.CompilerParams(vmem_limit_bytes=mebibytes << 20)


def cost(micros):
    return pl.CostEstimate(flops=int(micros * 1e8), bytes_accessed=int(micros * 1e6), transcendentals=0)


def part_of(flip):
    def index(i):
        _, _, x, core = here()
        return place_of(first(x, core) ^ flip, i, core)

    return index


def rows_of(spot, pair):
    z, y, _, core = here()
    there_y = place_of(first(y, core) ^ (spot >> 1), pair >> 1, core)
    there_z = place_of(first(z, core) ^ (spot & 1), pair & 1, core)
    return there_z * RING + there_y


def spread_rows(rows, qterm, oterm, outs, base):
    width = qterm.shape[1]
    for spot in range(4):
        for pair in range(4):
            at = pl.ds(pl.multiple_of(rows_of(spot, pair) * rows, rows), rows)
            outs[spot][base + pair, :, :width] = qterm[at, :]
            outs[spot][base + pair, :, width:] = oterm[at, :]


def over_tokens(low, other):
    value = jnp.dot(low[0], other, preferred_element_type=F32)
    return value + jnp.dot(low[1], other, preferred_element_type=F32)


def blocks_kernel(rows, flip, qlow, olow, cot, heads, outs, qterm, oterm):
    for part in range(2):
        index = part_of(flip)(part)
        for low, other, term in ((qlow, cot, qterm), (olow, heads, oterm)):
            width = term.shape[1]
            at = pl.ds(pl.multiple_of(index * width, 128), width)
            term[...] = over_tokens(low, other[:, at])
        spread_rows(rows, qterm, oterm, outs, 4 * part)


def front_kernel(rows, latent, mix, qbasis, obasis, cot, heads, *refs):
    qlow, olow, outs = refs[0], refs[1], refs[2:6]
    xs, ms, qs, os, qfar, ofar, total, qterm, oterm, sems = refs[6:]
    copies, waits = [], {}

    def bring(key, source, target):
        waits.setdefault(key, []).append(len(copies))
        copies.append(pltpu.make_async_copy(source, target, sems.at[len(copies)]))

    for name, tokens, basis, inside, beside in (("x", latent, qbasis, xs, qs), ("m", mix, obasis, ms, os)):
        wide = tokens.shape[1] // STEPS
        for k in range(STEPS):
            at = pl.ds(k * wide, wide)
            bring((name, k), basis.at[at, :], beside.at[at, :])
            bring((name, k), tokens.at[:, at], inside.at[:, at])
    for source, target in ((cot, qfar), (heads, ofar)):
        width = target.shape[2]
        for part in range(2):
            at = pl.ds(pl.multiple_of(part_of(1)(part) * width, 128), width)
            bring(part, source.at[:, at], target.at[part])
    begun = 0

    def ahead(upto):
        nonlocal begun
        while begun < min(upto, len(copies)):
            copies[begun].start()
            begun += 1

    def ready(key):
        for k in waits[key]:
            copies[k].wait()
        ahead(max(waits[key]) + 1 + AHEAD)

    apart = lax.axis_index("fs") >= 0
    ahead(AHEAD)
    for name, inside, beside, low in (("x", xs, qs, qlow), ("m", ms, os, olow)):
        wide = inside.shape[1] // STEPS
        for k in range(STEPS):

            @pl.when(apart)
            def _():
                ready((name, k))
                term = jnp.dot(
                    inside[:, k * wide : (k + 1) * wide],
                    beside[k * wide : (k + 1) * wide, :],
                    preferred_element_type=F32,
                )
                if k > 0:
                    term += total[...]
                if k < STEPS - 1:
                    total[...] = term
                else:
                    high, rest = halves(term)
                    low[0] = high.T
                    low[1] = rest.T

    for part in range(2):

        @pl.when(apart)
        def _():
            ready(part)
            qterm[...] = over_tokens(qlow, qfar[part])
            oterm[...] = over_tokens(olow, ofar[part])
            spread_rows(rows, qterm, oterm, outs, 4 * part)


def front(latent, mix, qbasis, obasis, cot, heads):
    tokens, rank = latent.shape[0], qbasis.shape[1]
    rows = rank // (RING * RING)
    qwide, owide = cot.shape[1] // RING, heads.shape[1] // RING
    low = jax.ShapeDtypeStruct((2, rank, tokens), BF16)
    kept = [jax.ShapeDtypeStruct((2, tokens, w), BF16) for w in (qwide, owide)]
    block = jax.ShapeDtypeStruct((8, rows, qwide + owide), F32)
    return pl.pallas_call(
        functools.partial(front_kernel, rows),
        in_specs=[pl.BlockSpec(memory_space=pltpu.HBM)] * 6,
        out_shape=[low, low] + [block] * 4,
        scratch_shapes=[pltpu.VMEM(a.shape, BF16) for a in (latent, mix, qbasis, obasis, *kept)]
        + [pltpu.VMEM((tokens, rank), F32)]
        + [pltpu.VMEM((rank, w), F32) for w in (qwide, owide)]
        + [pltpu.SemaphoreType.DMA((4 * STEPS + 4,))],
        compiler_params=params(FRONT),
        cost_estimate=cost(7),
        name="front",
    )(latent, mix, qbasis, obasis, cot, heads)


def near_kernel(rows, qlow, olow, cot, heads, *refs):
    blocks_kernel(rows, 0, qlow, olow, cot, heads, refs[:4], *refs[4:])


def near_blocks(qlow, olow, cot, heads):
    rank = qlow.shape[1]
    rows = rank // (RING * RING)
    qwide, owide = cot.shape[1] // RING, heads.shape[1] // RING
    block = jax.ShapeDtypeStruct((8, rows, qwide + owide), F32)
    return pl.pallas_call(
        functools.partial(near_kernel, rows),
        out_shape=[block] * 4,
        scratch_shapes=[pltpu.VMEM((rank, w), F32) for w in (qwide, owide)],
        compiler_params=params(FAR),
        cost_estimate=cost(2),
        name="near",
    )(qlow, olow, cot, heads)


def tree(values):
    while len(values) > 1:
        values = [a + b for a, b in zip(values[::2], values[1::2])]
    return values[0]


def lanes(value):
    _, wide = value.shape
    total = jnp.sum(value, axis=0, keepdims=True)
    return sum(total[:, k : k + 128] for k in range(0, wide, 128))


def total_kernel(*refs):
    value = tree([r[...] for r in refs[:8]])
    for half in range(2):
        refs[8 + half][...] = value[4 * half : 4 * half + 4]


def squares_kernel(split, *refs):
    proj, squares = refs[4:]
    for half in range(2):
        proj[4 * half : 4 * half + 4] = refs[2 * half][...] + refs[2 * half + 1][...]
    value = proj[...]
    value = value.reshape(value.shape[0] * value.shape[1], value.shape[2])
    square = value * value
    mine = jnp.concatenate([lanes(square[:, :split]), lanes(square[:, split:])], axis=0)
    squares[...] = jnp.broadcast_to(mine, squares.shape)


def total(terms):
    shape = terms[0].shape
    return pl.pallas_call(
        total_kernel,
        out_shape=[jax.ShapeDtypeStruct((4, *shape[1:]), F32)] * 2,
        compiler_params=params(10),
        cost_estimate=cost(0.5),
        name="total",
    )(*terms)


def total_squares(terms, split):
    return pl.pallas_call(
        functools.partial(squares_kernel, split),
        out_shape=[
            jax.ShapeDtypeStruct((8, *terms[0].shape[1:]), F32),
            jax.ShapeDtypeStruct((8, 2, 128), F32),
        ],
        compiler_params=params(10),
        cost_estimate=cost(0.5),
        name="total_squares",
    )(*terms)


def moments_kernel(qmean, qvar, omean, ovar, out):
    _, _, x, core = here()
    for part in range(2):
        index = place_of(first(x, core), part, core)
        start = 0
        for source in ((qmean, qvar), (omean, ovar)):
            width = source[0].shape[1] // RING
            at = pl.ds(pl.multiple_of(index * width, 128), width)
            for which in range(2):
                out[which, part, :, start : start + width] = source[which][:, at]
            start += width


def moments(qmean, qvar, omean, ovar):
    wide = (qmean.shape[1] + omean.shape[1]) // RING
    return pl.pallas_call(
        moments_kernel,
        out_shape=jax.ShapeDtypeStruct((2, 2, qmean.shape[0], wide), F32),
        compiler_params=params(4),
        cost_estimate=cost(1),
        name="moments",
    )(qmean, qvar, omean, ovar)


def direction_kernel(split, counts, mine, other, proj, *refs):
    moved, out = refs[:4], refs[4]
    z, y, _, core = here()
    own = second(y, core) * 2 + second(z, core)
    sums = jnp.sum(mine[...], axis=0) + jnp.sum(other[...], axis=0)
    sums = jnp.sum(sums, axis=1, keepdims=True)
    scales = [1.0 / jnp.maximum(jnp.sqrt(sums[k : k + 1] / counts[k]), 1.0) for k in range(2)]
    for offset in range(4):
        for part in range(2):
            shard = part * 4 + (own ^ offset)
            for k, at in enumerate((slice(0, split), slice(split, None))):
                scaled = scales[k] * proj[shard, :, at]
                new_mean = 0.8 * moved[offset][0, part, :, at] + 0.2 * scaled
                new_var = 0.9 * moved[offset][1, part, :, at] + 0.1 * scaled * scaled
                out[shard, :, at] = new_mean / jnp.sqrt(new_var)


def direction(mine, other, proj, moved, split, counts):
    return pl.pallas_call(
        functools.partial(direction_kernel, split, counts),
        out_shape=jax.ShapeDtypeStruct(proj.shape, F32),
        compiler_params=params(6),
        cost_estimate=cost(1.5),
        name="direction",
    )(mine, other, proj, *moved)


def late_kernel(rows, split, aliased, *refs):
    dirs, (qbasis, obasis, qweight, oweight) = refs[:4], refs[4:8]
    outs, scratch = refs[8 + aliased : 12 + aliased], refs[12 + aliased :]
    qstep, ostep, qcopy, ocopy = outs
    for spot in range(4):
        for pair in range(4):
            at = pl.ds(pl.multiple_of(rows_of(spot, pair) * rows, rows), rows)
            for ref, value in zip(scratch, halves(dirs[spot][pair])):
                ref[at, :] = value
    wide = scratch[0].shape[1]
    for basis, at, weight, step, copy in (
        (qbasis, slice(0, split), qweight, qstep, qcopy),
        (obasis, slice(split, wide), oweight, ostep, ocopy),
    ):
        value = jnp.dot(basis[...], scratch[0][:, at], preferred_element_type=F32)
        value += jnp.dot(basis[...], scratch[1][:, at], preferred_element_type=F32)
        step[...] = value
        copy[...] = (weight[...] - 0.05 * value).astype(BF16)


def late(dirs, qbasis, obasis, qweight, oweight, split, flip, before=()):
    _, rows, wide = dirs[0].shape
    rank = qbasis.shape[1]
    index = part_of(flip)
    qspec = pl.BlockSpec((qweight.shape[0], split), lambda i: (0, index(i)))
    ospec = pl.BlockSpec((oweight.shape[0], wide - split), lambda i: (0, index(i)))
    return pl.pallas_call(
        functools.partial(late_kernel, rows, split, len(before)),
        grid=(2,),
        in_specs=[pl.BlockSpec((4, rows, wide), lambda i: (i, 0, 0))] * 4
        + [
            pl.BlockSpec((qweight.shape[0], rank), lambda i: (lax.axis_index("fs"), 0)),
            pl.BlockSpec((oweight.shape[0], rank), lambda i: (lax.axis_index("fs"), 0)),
            qspec,
            ospec,
        ]
        + [pl.BlockSpec(memory_space=pl.ANY)] * len(before),
        out_specs=[qspec, ospec, qspec, ospec],
        out_shape=[
            jax.ShapeDtypeStruct(qweight.shape, F32),
            jax.ShapeDtypeStruct(oweight.shape, F32),
            jax.ShapeDtypeStruct(qweight.shape, BF16),
            jax.ShapeDtypeStruct(oweight.shape, BF16),
        ],
        scratch_shapes=[pltpu.VMEM((rank, wide), BF16)] * 2,
        input_output_aliases={8 + k: k for k in range(len(before))},
        compiler_params=params(12),
        cost_estimate=cost(2),
    )(*dirs, qbasis, obasis, qweight, oweight, *before)


def swap(value, phase, offset):
    return lax.ppermute(value, AXES, partners(phase, offset))


def on_device(
    saved_latent,
    query_cotangent,
    mix_cotangent,
    head_outputs,
    query_weight,
    out_weight,
    query_basis,
    out_basis,
    query_mean,
    query_var,
    out_mean,
    out_var,
):
    rank, cores = query_basis.shape[1], lax.axis_size("tp")
    split = query_cotangent.shape[1] // RING
    counts = (
        float(rank * query_cotangent.shape[1] * cores),
        float(rank * head_outputs.shape[1] * cores),
    )
    qlow, olow, *far = front(
        saved_latent, mix_cotangent, query_basis, out_basis, query_cotangent, head_outputs
    )
    near = near_blocks(qlow, olow, query_cotangent, head_outputs)
    held = moments(query_mean, query_var, out_mean, out_var)
    came = {}
    for k in GATHER:
        came[k] = swap(far[k - 4] if k > 3 else near[k], 1, k)
    moved = [held]
    for k in (1, 2, 3):
        moved.append(swap(held, 2, k))
    chains = list(total([near[0]] + [came[k] for k in range(1, 8)]))
    for step in range(3):
        others = []
        for v, order in zip(chains, ORDERS):
            others.append(swap(v, 2, order[step]))
        if step < 2:
            chains = [v + w for v, w in zip(chains, others)]
    last = [v for pair in zip(chains, others) for v in pair]
    proj, squares = total_squares(last, split)
    mine = lax.all_to_all(squares, AXES, 0, 0, tiled=True, axis_index_groups=first_groups())
    other = lax.ppermute(mine, "tp", [(0, 1), (1, 0)])
    dirs = direction(mine, other, proj, moved, split, counts)
    spread = {0: dirs}
    for k in SPREAD:
        spread[k] = swap(dirs, 1, k)
    spread = [spread[k] for k in range(8)]
    steps = late(spread[:4], query_basis, out_basis, query_weight, out_weight, split, 0)
    return tuple(late(spread[4:], query_basis, out_basis, query_weight, out_weight, split, 1, steps))


def solution(mesh):
    placed = (
        P(("fs", "rep"), None),
        P(("fs", "rep"), "tp"),
        P(("fs", "rep"), None),
        P(("fs", "rep"), "tp"),
        P("fs", "tp"),
        P("fs", "tp"),
        P(),
        P(),
        P("fs", "tp"),
        P("fs", "tp"),
        P("fs", "tp"),
        P("fs", "tp"),
    )
    return jax.shard_map(
        on_device,
        mesh=mesh,
        in_specs=placed,
        out_specs=(P("fs", "tp"), P("fs", "tp"), P("fs", "tp"), P("fs", "tp")),
        check_vma=False,
    )
```
